32 devices in a mesh: ep: 8 (over z, core), tp: 4 (over y, x).
Axes of the slice: x: 2, y: 2, z: 4, core: 2. Of those that a mesh axis runs over, the one named last changes fastest.
Arguments:
- queries: bfloat16 [4096, 1024], P('ep', 'tp'), may hold values from -9 to 9
- keys: bfloat16 [4096, 128], P('ep'), may hold values from -6 to 6
- values: bfloat16 [4096, 128], P('ep'), may hold values from -6 to 6
- sink_logits: float32 [16], P('tp'), may hold values from 2 to 7
- out_weight: bfloat16 [1024, 2048], P(None, 'tp'), may hold values from -0.8984375 to 0.8984375
- expert_input: bfloat16 [2048, 2048], P('ep'), may hold values from -6 to 6
- norm_gain: float32 [2048], replicated, may hold values from 0.1 to 1.9
- routes: int32 [2048, 2], P('ep'), may hold values from 0 to 7, all different within a row; in each aligned block of 256 rows (0 to 255, 256 to 511, ...) at most 128 rows name the same one
- route_weights: float32 [2048, 2], P('ep'), may hold values from 0.1 to 1
- gate_weight: bfloat16 [8, 2048, 4096], P('ep', None, 'tp'), may hold values from -0.125 to 0.125
- up_weight: bfloat16 [8, 2048, 4096], P('ep', None, 'tp'), may hold values from -0.125 to 0.125
- down_weight: bfloat16 [8, 4096, 2048], P('ep', 'tp'), may hold values from -0.09375 to 0.09375
Outputs:
- attn_out: bfloat16 [4096, 2048], P('ep', 'tp')
- expert_out: bfloat16 [2048, 2048], P('ep', 'tp')
The draws below stay inside these ranges and needn't reach their ends.
Inputs may be any that keep to these rules, and one draw needn't show every extreme that they name: `routes`: each row names 2 different experts. Within the rows of one index of ep (aligned blocks of 256 rows) no expert is named by more than 128 rows, and in some blocks one expert is named by exactly 128 rows.
All inputs are finite; a program needn't handle non-finite values.
Results may differ from the reference program's by a relative error of at most 0.015.
Values may be sent and summed in bfloat16 or wider, within the bound.
No kernel may reach another device: no remote copies, remote signals or barrier semaphores. Data moves between devices by JAX's collectives and lax.ppermute only.
A program may use at most 64 MiB of HBM per device.

```python
import math
import jax
import jax.numpy as jnp
import numpy as np
from jax import lax

D = 2048
HEADS = 16
KV = 2
HD = 64
WINDOW = 128
FF = 4096
TOPK = 2
TOK_E_DEV = 256
TOK_A = 4096
TOK_E = 2048
EXPERTS = 8
CAP = 128
N_EP = 8
N_TP = 4


def draw_queries(key, part):
    sample = jnp.clip(jax.random.normal(key, (TOK_A, HEADS * HD), jnp.float32) * 1.5, -9.0, 9.0)
    return sample.astype(jnp.bfloat16)


def draw_keys(key, part):
    sample = jnp.clip(jax.random.normal(key, (TOK_A, KV * HD), jnp.float32), -6.0, 6.0)
    return sample.astype(jnp.bfloat16)


def block_levels(key, extent, pieces, least, top_value):
    gain, own = 1.0, jax.random.fold_in(key, 6)
    for axis_at, parts in pieces:
        draws = jnp.exp(jax.random.uniform(jax.random.fold_in(own, axis_at), (parts,), jnp.float32, least / len(pieces), top_value / len(pieces)))
        gain = gain * jnp.repeat(draws, extent[axis_at] // parts).reshape([-1 if axis == axis_at else 1 for axis in range(len(extent))])
    return gain


def deal_out(key, own, number, rows, count, top, limit, lean):
    ranking = jax.random.permutation(key, count)
    packed, usual = shares(count, rows * top, limit, lean, True), shares(count, rows * top, limit, lean, False)
    places = jnp.arange(count)

    def named(lengths, turn):
        used = int((lengths > 0).sum())
        fixed = max(1, used // 4)
        moved = fixed + (places - fixed + turn * (used - fixed)) % max(1, count - fixed)
        return jnp.zeros((count,), jnp.int32).at[ranking[jnp.where(places < fixed, places, moved)]].set(jnp.asarray(lengths, jnp.int32))

    lengths = jnp.where(number % 4 == 0, named(packed, number // 4), named(usual, number - number // 4 - 1))
    mixed = jax.random.permutation(jax.random.fold_in(own, 3), count)
    source_of, receiver = mixed[0:count // 2 * 2:2], mixed[1:count // 2 * 2:2]
    margin = jnp.minimum(lengths[source_of] - 1, limit - lengths[receiver]) // 2
    margin = jnp.where((source_of == ranking[0]) | (receiver == ranking[0]) | (lengths[receiver] == 0), 0, jnp.maximum(margin, 0))
    moved = jax.random.randint(jax.random.fold_in(own, 4), (count // 2,), 0, 1 << 20) % (margin + 1)
    lengths = lengths.at[source_of].add(-moved).at[receiver].add(moved)
    members = jnp.searchsorted(jnp.cumsum(lengths), jnp.arange(rows * top), side="right").astype(jnp.int32)
    table = members.reshape(top, rows).T
    table = table[jax.random.permutation(jax.random.fold_in(own, 1), rows)]
    turn = jax.random.randint(jax.random.fold_in(own, 2), (rows, 1), 0, top)
    return jnp.take_along_axis(table, (jnp.arange(top)[None, :] + turn) % top, axis=1)


def shares(count, total, bound, slope, full):
    loads = [(1 << 20) // math.isqrt(grade ** slope) + 1 for grade in range(1, count + 1)]
    largest = bound if full else min(bound, max(-(-total // count), total * loads[0] // sum(loads)))
    least = 1 if total - largest >= count - 1 else 0
    given, rest = [largest] + [least] * (count - 1), total - largest - least * (count - 1)
    while rest > 0:
        free = [i for i in range(1, count) if given[i] < largest] or [i for i in range(1, count) if given[i] < bound]
        whole, remaining = sum([loads[i] for i in free]), rest
        for i in free:
            addition = min(bound - given[i], max(1, remaining * loads[i] // whole), rest)
            given[i] = given[i] + addition
            rest = rest - addition
    return np.array(given)


def noise(key, extent, width, most, split=(), kind=jnp.bfloat16):
    loudness = block_levels(key, extent, split, -0.22, 0.18) if split else 1.0
    values = jax.random.normal(key, extent, jnp.float32) * width * loudness
    return jnp.minimum(jnp.maximum(values, -most), most).astype(kind)


def setup_inputs(seed: int = 0) -> dict:
    streams_of = jax.random.split(jax.random.key(seed), 13)
    queries = draw_queries(jax.random.fold_in(streams_of[12], 71), 0)
    keys = draw_keys(jax.random.fold_in(streams_of[12], 71), 0)
    values = noise(streams_of[2], (TOK_A, KV * HD), 1.0, 6.0, ((0, 8),))
    sink_logits = jnp.clip(2.0 + 5.0 * jax.random.uniform(streams_of[3], (HEADS,), jnp.float32) ** block_levels(streams_of[3], (HEADS,), ((0, 4),), -0.2, 0.2), 2.0, 7.0)
    out_weight = noise(streams_of[4], (HEADS * HD, D), 0.15, 0.8984375, ((1, 4),))
    expert_input = noise(streams_of[5], (TOK_E, D), 1.0, 6.0, ((0, 8),))
    norm_gain = jnp.clip(1.0 + 0.18 * jax.random.normal(streams_of[6], (D,), jnp.float32), 0.1, 1.9)
    routes_keys = jax.random.split(jax.random.fold_in(streams_of[7], 1), TOK_E // TOK_E_DEV)
    routes_turns = jax.random.permutation(jax.random.fold_in(streams_of[7], 3), TOK_E // TOK_E_DEV)
    routes = jax.vmap(lambda own, number: deal_out(jax.random.fold_in(streams_of[7], 2), own, number, TOK_E_DEV, EXPERTS, TOPK, CAP, 1))(routes_keys, routes_turns).reshape((TOK_E, TOPK))
    route_weights = jnp.clip(0.1 + 0.9 * jax.random.uniform(streams_of[8], (TOK_E, TOPK), jnp.float32) ** block_levels(streams_of[8], (TOK_E, TOPK), ((0, 8),), -0.2, 0.2), 0.1, 1.0)
    gate_weight = noise(streams_of[9], (EXPERTS, D, FF), D ** -0.5, 0.125, ((0, 8), (2, 4)))
    up_weight = noise(streams_of[10], (EXPERTS, D, FF), D ** -0.5, 0.125, ((0, 8), (2, 4)))
    down_weight = noise(streams_of[11], (EXPERTS, FF, D), FF ** -0.5, 0.09375, ((0, 8), (1, 4)))
    return {"queries": queries, "keys": keys, "values": values, "sink_logits": sink_logits, "out_weight": out_weight, "expert_input": expert_input, "norm_gain": norm_gain, "routes": routes, "route_weights": route_weights, "gate_weight": gate_weight, "up_weight": up_weight, "down_weight": down_weight}


rms_eps = 1e-06
mask_value = -1e+30

def rotate_heads(values_in, positions):
    half_dim = values_in.shape[-1] // 2
    inv_freq = 10000.0 ** (-jnp.arange(half_dim, dtype=jnp.float32) * (2.0 / values_in.shape[-1]))
    angles = positions[:, None] * inv_freq[None, :]
    cosine_table = jnp.cos(angles)[:, None, :]
    sine_table = jnp.sin(angles)[:, None, :]
    first_half = values_in[..., :half_dim]
    second_half = values_in[..., half_dim:]
    return jnp.concatenate([first_half * cosine_table - second_half * sine_table, second_half * cosine_table + first_half * sine_table], axis=-1)

def one_head(operands):
    head_query, head_key, head_value, head_sink = operands
    tokens_all = head_query.shape[0]
    blocks = tokens_all // WINDOW
    zero_rim = jnp.zeros((WINDOW, HD), head_key.dtype)

    def band_of(source):
        padded = jnp.concatenate([zero_rim, source], axis=0)
        earlier = padded[:tokens_all].reshape(blocks, WINDOW, HD)
        current = padded[WINDOW:].reshape(blocks, WINDOW, HD)
        return jnp.concatenate([earlier, current], axis=1).astype(jnp.float32)
    query_blocks = head_query.reshape(blocks, WINDOW, HD).astype(jnp.float32)
    scores = jnp.einsum('nqd,nkd->nqk', query_blocks, band_of(head_key)) * HD ** (-0.5)
    block_start = jnp.arange(blocks, dtype=jnp.int32)[:, None, None] * WINDOW
    query_pos = block_start + jnp.arange(WINDOW, dtype=jnp.int32)[None, :, None]
    key_pos = block_start - WINDOW + jnp.arange(2 * WINDOW, dtype=jnp.int32)[None, None, :]
    distance = query_pos - key_pos
    allowed = (distance >= 0) & (distance < WINDOW) & (key_pos >= 0)
    scores = jnp.where(allowed, scores, mask_value)
    row_top = jnp.maximum(lax.optimization_barrier(jnp.max(scores, axis=-1)), head_sink)
    exp_scores = jnp.exp(scores - row_top[..., None])
    row_total = lax.optimization_barrier(jnp.sum(exp_scores, axis=-1)) + jnp.exp(head_sink - row_top)
    weights = (exp_scores / row_total[..., None]).astype(jnp.bfloat16)
    head_mix = jnp.einsum('nqk,nkd->nqd', weights.astype(jnp.float32), band_of(head_value))
    return head_mix.astype(jnp.bfloat16).reshape(tokens_all, HD)

def reference(queries, keys, values, sink_logits, out_weight, expert_input, norm_gain, routes, route_weights, gate_weight, up_weight, down_weight):
    tokens_all = queries.shape[0]
    positions = jnp.arange(tokens_all, dtype=jnp.int32).astype(jnp.float32)
    query_rot = rotate_heads(queries.astype(jnp.float32).reshape(tokens_all, HEADS, HD), positions).astype(jnp.bfloat16)
    key_rot = rotate_heads(keys.astype(jnp.float32).reshape(tokens_all, KV, HD), positions).astype(jnp.bfloat16)
    value_heads = values.reshape(tokens_all, KV, HD)
    group_size = HEADS // KV
    query_t = jnp.transpose(query_rot, (1, 0, 2))
    key_t = jnp.repeat(jnp.transpose(key_rot, (1, 0, 2)), group_size, axis=0)
    value_t = jnp.repeat(jnp.transpose(value_heads, (1, 0, 2)), group_size, axis=0)
    head_outputs = lax.map(one_head, (query_t, key_t, value_t, sink_logits.astype(jnp.float32)))
    head_mix = jnp.transpose(head_outputs, (1, 0, 2)).reshape(tokens_all, HEADS * HD)
    attn_out = jnp.dot(head_mix, out_weight, preferred_element_type=jnp.float32).astype(jnp.bfloat16)
    token_rows = expert_input.shape[0]
    input_wide = expert_input.astype(jnp.float32)
    inv_rms = lax.rsqrt(lax.optimization_barrier(jnp.mean(input_wide * input_wide, axis=-1, keepdims=True)) + rms_eps)
    normed = (input_wide * inv_rms * norm_gain.astype(jnp.float32)[None, :]).astype(jnp.bfloat16)
    grouped = routes.reshape(N_EP, TOK_E_DEV * TOPK).astype(jnp.int32)
    one_hot = (grouped[..., None] == jnp.arange(EXPERTS, dtype=jnp.int32)[None, None, :]).astype(jnp.int32)
    route_rank = lax.optimization_barrier(jnp.sum(jnp.cumsum(one_hot, axis=1) * one_hot, axis=-1)) - 1
    source_block = jnp.arange(N_EP, dtype=jnp.int32)[:, None]
    slot_index = (grouped * (N_EP * CAP) + source_block * CAP + route_rank).reshape(-1).astype(jnp.int32)
    route_token = (jnp.arange(token_rows * TOPK, dtype=jnp.int32) // TOPK).astype(jnp.int32)
    slot_table = jnp.full((EXPERTS * N_EP * CAP,), token_rows, jnp.int32).at[slot_index].set(route_token).reshape(EXPERTS, N_EP * CAP)
    padded = jnp.concatenate([normed, jnp.zeros((1, D), normed.dtype)], axis=0)
    width_block = FF // N_TP

    def one_expert(operands):
        table_row, gate_mat, up_mat, down_mat = operands
        rows_in = padded[table_row]
        gate_acc = jnp.dot(rows_in, gate_mat, preferred_element_type=jnp.float32)
        up_acc = jnp.dot(rows_in, up_mat, preferred_element_type=jnp.float32)
        hidden = (jax.nn.silu(gate_acc) * up_acc).astype(jnp.bfloat16)
        block_parts = jnp.einsum('sjf,jfd->jsd', hidden.reshape(-1, N_TP, width_block).astype(jnp.float32), down_mat.reshape(N_TP, width_block, D).astype(jnp.float32)).astype(jnp.bfloat16)
        return lax.optimization_barrier(jnp.sum(block_parts.astype(jnp.float32), axis=0)).astype(jnp.bfloat16)
    outputs = lax.map(one_expert, (slot_table, gate_weight, up_weight, down_weight))
    picked = outputs.reshape(-1, D)[slot_index].astype(jnp.float32)
    expert_out = lax.optimization_barrier(jnp.sum(picked.reshape(token_rows, TOPK, D) * route_weights.astype(jnp.float32)[..., None], axis=1)).astype(jnp.bfloat16)
    return (attn_out, expert_out)
```

```python
import functools

import jax
import jax.numpy as jnp
import numpy as np
from jax import lax
from jax.experimental import pallas as pl
from jax.experimental.pallas import tpu as pltpu
from jax.sharding import PartitionSpec as P


HEADS = 16
KV = 2
HD = 64
WINDOW = 128


rms_eps = 1e-06
mask_value = -1e30


def passed_along(value, axis, steps):
    count = lax.axis_size(axis)
    first, last = (max(0, -steps), min(count, count - steps))
    return lax.ppermute(value, axis, [(source, source + steps) for source in range(first, last)])


def rotate_heads(values_in, positions):
    half_dim = values_in.shape[-1] // 2
    inv_freq = 10000.0 ** (-jnp.arange(half_dim, dtype=jnp.float32) * (2.0 / values_in.shape[-1]))
    angles = positions[:, None] * inv_freq[None, :]
    cosine_table = jnp.cos(angles)[:, None, :]
    sine_table = jnp.sin(angles)[:, None, :]
    first_half = values_in[..., :half_dim]
    second_half = values_in[..., half_dim:]
    return jnp.concatenate(
        [
            first_half * cosine_table - second_half * sine_table,
            second_half * cosine_table + first_half * sine_table,
        ],
        axis=-1,
    )


def local_general(
    queries,
    keys,
    values,
    sink_logits,
    out_weight,
    expert_input,
    norm_gain,
    routes,
    route_weights,
    gate_weight,
    up_weight,
    down_weight,
):
    seq_rows = queries.shape[0]
    heads_here = queries.shape[1] // HD
    group_size = HEADS // KV
    kv_here = max(1, heads_here // group_size)
    heads_per_kv = heads_here // kv_here
    kv_first = lax.axis_index("tp") * heads_here // group_size
    key_local = lax.dynamic_slice_in_dim(keys, kv_first * HD, kv_here * HD, 1)
    value_local = lax.dynamic_slice_in_dim(values, kv_first * HD, kv_here * HD, 1)
    offset = lax.axis_index("ep") * seq_rows
    positions = (offset + jnp.arange(seq_rows, dtype=jnp.int32)).astype(jnp.float32)
    query_rot = rotate_heads(
        queries.astype(jnp.float32).reshape(seq_rows, heads_here, HD), positions
    ).astype(jnp.bfloat16)
    key_rot = rotate_heads(
        key_local.astype(jnp.float32).reshape(seq_rows, kv_here, HD), positions
    ).astype(jnp.bfloat16)
    value_heads = value_local.reshape(seq_rows, kv_here, HD)
    rim_pair = jnp.concatenate(
        [
            key_rot.reshape(seq_rows, kv_here * HD)[seq_rows - WINDOW :],
            value_local[seq_rows - WINDOW :],
        ],
        axis=1,
    )
    rim_pair = passed_along(rim_pair, "ep", 1)
    rim_key = rim_pair[:, : kv_here * HD].reshape(WINDOW, kv_here, HD)
    rim_value = rim_pair[:, kv_here * HD :].reshape(WINDOW, kv_here, HD)
    blocks = seq_rows // WINDOW

    def band_of(rim_part, local_part):
        padded = jnp.concatenate([rim_part, local_part], axis=0)
        earlier = padded[:seq_rows].reshape(blocks, WINDOW, kv_here, HD)
        current = padded[WINDOW:].reshape(blocks, WINDOW, kv_here, HD)
        return jnp.concatenate([earlier, current], axis=1)

    key_band = band_of(rim_key, key_rot)
    value_band = band_of(rim_value, value_heads)
    query_blocks = query_rot.reshape(blocks, WINDOW, kv_here, heads_per_kv, HD)
    scores = jnp.einsum(
        "nqhgd,nkhd->nhgqk", query_blocks, key_band, preferred_element_type=jnp.float32
    ) * HD ** (-0.5)
    block_start = offset + jnp.arange(blocks, dtype=jnp.int32)[:, None, None] * WINDOW
    query_pos = block_start + jnp.arange(WINDOW, dtype=jnp.int32)[None, :, None]
    key_pos = block_start - WINDOW + jnp.arange(2 * WINDOW, dtype=jnp.int32)[None, None, :]
    distance = query_pos - key_pos
    allowed = (distance >= 0) & (distance < WINDOW) & (key_pos >= 0)
    scores = jnp.where(allowed[:, None, None], scores, mask_value)
    sink_row = sink_logits.reshape(1, kv_here, heads_per_kv, 1)
    row_top = jnp.maximum(jnp.max(scores, axis=-1), sink_row)
    exp_scores = jnp.exp(scores - row_top[..., None])
    row_total = jnp.sum(exp_scores, axis=-1) + jnp.exp(sink_row - row_top)
    weights = (exp_scores / row_total[..., None]).astype(jnp.bfloat16)
    head_mix = jnp.einsum(
        "nhgqk,nkhd->nqhgd", weights, value_band, preferred_element_type=jnp.float32
    )
    head_mix = head_mix.astype(jnp.bfloat16).reshape(seq_rows, heads_here * HD)
    attn_out = jnp.dot(
        lax.all_gather(head_mix, "tp", axis=1, tiled=True),
        out_weight,
        preferred_element_type=jnp.float32,
    ).astype(jnp.bfloat16)
    token_rows = expert_input.shape[0]
    top_count = routes.shape[1]
    expert_count = lax.axis_size("ep")
    capacity = 2 * top_count * token_rows // expert_count
    slot_total = expert_count * capacity
    input_wide = expert_input.astype(jnp.float32)
    inv_rms = lax.rsqrt(jnp.mean(input_wide * input_wide, axis=-1, keepdims=True) + rms_eps)
    normed = (input_wide * inv_rms * norm_gain[None, :]).astype(jnp.bfloat16)
    flat_expert = routes.reshape(-1)
    one_hot = (flat_expert[:, None] == jnp.arange(expert_count, dtype=jnp.int32)[None, :]).astype(
        jnp.int32
    )
    route_rank = jnp.sum(jnp.cumsum(one_hot, axis=0) * one_hot, axis=1) - 1
    slot_of_route = flat_expert * capacity + route_rank
    matches = slot_of_route[None, :] == jnp.arange(slot_total, dtype=jnp.int32)[:, None]
    route_token = jnp.arange(token_rows * top_count, dtype=jnp.int32) // top_count
    source_row = jnp.sum(jnp.where(matches, route_token[None, :] + 1, 0), axis=1) - 1
    occupied = source_row >= 0
    gate_local = gate_weight[0]
    up_local = up_weight[0]
    down_local = down_weight[0]
    column_count = normed.shape[1] // lax.axis_size("tp")
    own_columns = lax.dynamic_slice_in_dim(
        normed, lax.axis_index("tp") * column_count, column_count, 1
    )
    slot_rows = jnp.where(
        occupied[:, None],
        jnp.take(own_columns, jnp.maximum(source_row, 0), axis=0),
        jnp.zeros((), jnp.bfloat16),
    )
    outgoing = slot_rows.reshape(expert_count, capacity, column_count)
    arrived = lax.all_to_all(outgoing, "ep", split_axis=0, concat_axis=0, tiled=True)
    leading = arrived.shape[:2]
    portion = lax.all_gather(arrived, "tp", axis=2, tiled=True)
    flat_piece = portion.reshape(-1, portion.shape[2])
    gate_acc = jnp.dot(flat_piece, gate_local, preferred_element_type=jnp.float32)
    up_acc = jnp.dot(flat_piece, up_local, preferred_element_type=jnp.float32)
    hidden = (jax.nn.silu(gate_acc) * up_acc).astype(jnp.bfloat16)
    summed = lax.psum_scatter(
        lax.dot_general(
            down_local, hidden, (((0,), (1,)), ((), ())), preferred_element_type=jnp.float32
        ).astype(jnp.bfloat16),
        "tp",
        scatter_dimension=0,
        tiled=True,
    ).astype(jnp.float32)
    returned = summed.astype(jnp.bfloat16).reshape((summed.shape[0],) + leading)
    results_home = lax.all_to_all(returned, "ep", split_axis=1, concat_axis=1, tiled=True)
    home_flat = results_home.reshape(results_home.shape[0], -1)
    picked = jnp.take(home_flat, slot_of_route, axis=1).astype(jnp.float32)
    weighted = picked * route_weights.reshape(1, -1)
    combined = jnp.sum(weighted.reshape(results_home.shape[0], token_rows, top_count), axis=2)
    expert_out = combined.T.astype(jnp.bfloat16)
    return (attn_out, expert_out)


BF = jnp.bfloat16
F32 = jnp.float32
MIB = 1024 * 1024
LATE = 2
NEAR = 1


def dot(left, right):
    return jnp.dot(left, right, preferred_element_type=F32)


def quarter(index, width):
    return pl.ds(pl.multiple_of(index * width, width), width)


def kernel_params(limit_mib, **extra):
    return pltpu.CompilerParams(vmem_limit_bytes=limit_mib * MIB, **extra)


def in_hbm(*values):
    return [pltpu.with_memory_space_constraint(value, pltpu.HBM) for value in values]


def whole_specs(count):
    return [pl.BlockSpec(memory_space=pltpu.VMEM)] * count


def axes_here():
    first = 1 + lax.rem(lax.axis_index("ep"), 2)
    return first, 3 - first


def naming(routes, lanes):
    choices, tokens = routes.shape
    expert = lax.broadcasted_iota(jnp.int32, (lanes, tokens), 0)
    hit = routes[0:1, :] == expert
    for choice in range(1, choices):
        hit = hit | (routes[choice : choice + 1, :] == expert)
    named = jnp.where(hit, 1.0, 0.0).astype(BF)
    row = lax.broadcasted_iota(jnp.int32, (tokens, tokens), 0)
    column = lax.broadcasted_iota(jnp.int32, (tokens, tokens), 1)
    earlier = jnp.where(row < column, 1.0, 0.0).astype(BF)
    return jnp.where(hit, dot(named, earlier), -1.0)


def dispatch_kernel(capacity, chips, x_hbm, gain_hbm, routes_hbm, queries_hbm, keys_hbm, values_hbm, *refs):
    outs, (x, gain, routes, normed, slot_of, arrival) = refs[:-6], refs[-6:]
    lanes = keys_hbm.shape[1]
    tail = pl.ds(keys_hbm.shape[0] - WINDOW, WINDOW)
    rim, queries, keys, values = outs[-4:]
    moves = (
        (routes_hbm, routes),
        (x_hbm, x),
        (gain_hbm, gain),
        (keys_hbm.at[tail, :], rim.at[:, :lanes]),
        (values_hbm.at[tail, :], rim.at[:, lanes:]),
        (queries_hbm, queries),
        (keys_hbm, keys),
        (values_hbm, values),
    )
    copies = [pltpu.make_async_copy(s, d, arrival.at[i]) for i, (s, d) in enumerate(moves)]
    for copy in copies:
        copy.start()
    me = lax.axis_index("ep")
    chip, core = me // 2, lax.rem(me, 2)
    tokens = x.shape[0]
    copies[0].wait()
    slot_of[...] = naming(routes[...], slot_of.shape[0])
    copies[1].wait()
    copies[2].wait()
    wide = x[...].astype(F32)
    inv_rms = lax.rsqrt(jnp.mean(wide * wide, axis=-1, keepdims=True) + rms_eps)
    normed[...] = (wide * inv_rms * gain[...]).astype(BF)
    slot = lax.broadcasted_iota(jnp.int32, (capacity, tokens), 0).astype(F32)

    def chosen(expert):
        return jnp.where(slot_of[pl.ds(expert, 1), :] == slot, 1.0, 0.0).astype(BF)

    width = outs[0].shape[1]
    share = normed[:, quarter(lax.axis_index("tp"), width)]
    place = 0
    for step in range(chips - 1, -1, -1):
        for other in range(2):
            rows = share if step > NEAR else normed[...]
            expert = (chip ^ step) * 2 + (core ^ other)
            outs[place][...] = dot(chosen(expert), rows).astype(BF)
            place += 1
    for copy in copies[3:]:
        copy.wait()


def dispatch(x, gain, routes, queries, keys, values, capacity, chips, width):
    tokens, features = x.shape
    shapes = [(capacity, width if i < 2 * (chips - 1 - NEAR) else features) for i in range(2 * chips)]
    shapes += [(WINDOW, 2 * keys.shape[1]), queries.shape, keys.shape, values.shape]
    return pl.pallas_call(
        functools.partial(dispatch_kernel, capacity, chips),
        out_shape=[jax.ShapeDtypeStruct(s, BF) for s in shapes],
        in_specs=[pl.BlockSpec(memory_space=pltpu.HBM)] * 6,
        out_specs=whole_specs(len(shapes)),
        scratch_shapes=[
            pltpu.VMEM((tokens, features), BF),
            pltpu.VMEM((1, features), F32),
            pltpu.VMEM(routes.shape[::-1], jnp.int32),
            pltpu.VMEM((tokens, features), BF),
            pltpu.VMEM((8 * -(-2 * chips // 8), tokens), F32),
            pltpu.SemaphoreType.DMA((8,)),
        ],
        compiler_params=kernel_params(24),
        cost_estimate=pl.CostEstimate(
            flops=4 * capacity * tokens * features * 2, bytes_accessed=4 * MIB, transcendentals=0
        ),
        name="dispatch",
    )(*in_hbm(x, gain.reshape(1, -1), routes.T, queries, keys, values))


def experts_kernel(split, fetch, blocks, *refs):
    count = 4 if split else 2
    rows_in = refs[:count]
    x, hidden = refs[-2:]
    if not fetch:
        gate, up, down, mine_ref, second_ref, far_ref = refs[count:-2]
    else:
        gate_hbm, up_hbm, down_hbm, gate, up, down, mine_ref, second_ref, far_ref, arrival = refs[count:-2]
    here = lax.axis_index("tp")
    first, second = axes_here()
    width = mine_ref.shape[1]
    block = hidden.shape[1] // blocks
    parts = [pl.ds(step * block, block) for step in range(blocks)]
    quarters = [quarter(index, width) for index in (here ^ first, here ^ 3, here ^ second, here)]
    copies = []
    if fetch:
        for place, part in enumerate(parts):
            for source, target, row in ((gate_hbm, gate, 0), (up_hbm, up, 1)):
                copies.append(
                    pltpu.make_async_copy(
                        source.at[:, :, part], target.at[:, :, part], arrival.at[row, place]
                    )
                )
        for place, part in enumerate(quarters):
            copies.append(
                pltpu.make_async_copy(down_hbm.at[:, :, part], down.at[:, :, part], arrival.at[2, place])
            )
        for copy in copies:
            copy.start()
    if split:
        for ref, index in zip(rows_in, (here, here ^ first, here ^ second, here ^ 3)):
            x[:, quarter(index, width)] = ref[...]
    else:
        half = rows_in[0].shape[0]
        x[:half, :] = rows_in[0][...]
        x[half:, :] = rows_in[1][...]
    for place, part in enumerate(parts):
        for copy in copies[2 * place : 2 * place + 2]:
            copy.wait()
        gated = dot(x[...], gate[0, :, part])
        upped = dot(x[...], up[0, :, part])
        hidden[:, part] = (gated / (1.0 + jnp.exp(-gated)) * upped).astype(BF)
    for place, part in enumerate(quarters):
        for copy in copies[2 * blocks + place : 2 * blocks + place + 1]:
            copy.wait()
        product = dot(hidden[...], down[0, :, part]).astype(BF)
        if place < 2:
            far_ref[:, place * width : (place + 1) * width] = product
        else:
            (second_ref if place == 2 else mine_ref)[...] = product


def experts(rows_in, weights, width, blocks, fetch=False):
    split = len(rows_in) == 4
    rows = rows_in[0].shape[0] if split else 2 * rows_in[0].shape[0]
    _, features, hidden = weights[0].shape
    out_shape = [
        jax.ShapeDtypeStruct((rows, width), BF),
        jax.ShapeDtypeStruct((rows, width), BF),
        jax.ShapeDtypeStruct((rows, 2 * width), BF),
    ]
    scratch = [pltpu.VMEM((rows, features), BF), pltpu.VMEM((rows, hidden), BF)]
    weight_specs = whole_specs(3)
    if fetch:
        weights = in_hbm(*weights)
        out_shape = [jax.ShapeDtypeStruct(w.shape, w.dtype) for w in weights] + out_shape
        weight_specs = [pl.BlockSpec(memory_space=pltpu.HBM)] * 3
        scratch = [pltpu.SemaphoreType.DMA((3, max(4, blocks)))] + scratch
    return pl.pallas_call(
        functools.partial(experts_kernel, split, fetch, blocks),
        out_shape=out_shape,
        in_specs=whole_specs(len(rows_in)) + weight_specs,
        out_specs=whole_specs(len(out_shape)),
        scratch_shapes=scratch,
        compiler_params=kernel_params(24 if fetch else 8),
        cost_estimate=pl.CostEstimate(
            flops=6 * rows * features * hidden,
            bytes_accessed=6 * features * hidden,
            transcendentals=rows * hidden,
        ),
        name="experts",
    )(*rows_in, *weights)


def join_kernel(top_ref, bottom_ref, out_ref):
    rows = top_ref.shape[0]
    out_ref[:rows, :] = top_ref[...]
    out_ref[rows:, :] = bottom_ref[...]


def join(top, bottom):
    rows, columns = top.shape
    return pl.pallas_call(
        join_kernel,
        out_shape=jax.ShapeDtypeStruct((2 * rows, columns), top.dtype),
        in_specs=whole_specs(2),
        out_specs=pl.BlockSpec(memory_space=pltpu.VMEM),
        compiler_params=kernel_params(2),
        cost_estimate=pl.CostEstimate(flops=MIB, bytes_accessed=MIB, transcendentals=0),
        name="join",
    )(top, bottom)


def settle_kernel(mine_ref, near_ref, last_ref, same_ref, cross_ref):
    rows, width = same_ref.shape
    for out_ref, start in ((same_ref, 0), (cross_ref, rows)):
        part = pl.ds(start, rows)
        total = mine_ref[part, :].astype(F32) + near_ref[part, :width].astype(F32)
        out_ref[...] = (total + last_ref[part, :].astype(F32)).astype(BF)


def settle(mine, near, last):
    rows, width = mine.shape
    return pl.pallas_call(
        settle_kernel,
        out_shape=[jax.ShapeDtypeStruct((rows // 2, width), BF)] * 2,
        in_specs=whole_specs(3),
        out_specs=whole_specs(2),
        compiler_params=kernel_params(4),
        cost_estimate=pl.CostEstimate(flops=MIB, bytes_accessed=MIB, transcendentals=0),
        name="settle",
    )(mine, near, last)


def project_kernel(*refs):
    parts, (weight_ref, out_ref) = refs[:4], refs[4:]
    here = lax.axis_index("tp")
    first, second = axes_here()
    depth = parts[0].shape[1]
    total = None
    for ref, index in zip(parts, (here, here ^ first, here ^ second, here ^ 3)):
        term = dot(ref[...], weight_ref[quarter(index, depth), :])
        total = term if total is None else total + term
    out_ref[...] = total.astype(BF)


def project(parts, weight):
    rows, columns = parts[0].shape[0], weight.shape[1]
    return pl.pallas_call(
        project_kernel,
        out_shape=jax.ShapeDtypeStruct((rows, columns), BF),
        in_specs=whole_specs(5),
        out_specs=pl.BlockSpec(memory_space=pltpu.VMEM),
        compiler_params=kernel_params(8),
        cost_estimate=pl.CostEstimate(
            flops=2 * rows * weight.shape[0] * columns, bytes_accessed=3 * MIB, transcendentals=0
        ),
        name="project",
    )(*parts, weight)


def combine_kernel(steps, late, *refs):
    routes_ref, weights_ref = refs[:2]
    pieces, (sum_ref, high_ref, low_ref) = refs[2:-3], refs[-3:]
    me = lax.axis_index("ep")
    chip, core = me // 2, lax.rem(me, 2)
    routes = routes_ref[...]
    choices, tokens = routes.shape
    capacity = high_ref.shape[1] // (2 * late)
    slot_of = naming(routes, 128)
    row = lax.broadcasted_iota(jnp.int32, (128, tokens), 0)
    scale = jnp.zeros((128, tokens), F32)
    for choice in range(choices):
        scale = jnp.where(routes[choice : choice + 1, :] == row, weights_ref[choice : choice + 1, :], scale)
    slot_of = slot_of.T.astype(BF)
    scale = scale.T
    high = scale.astype(BF)
    low = (scale - high.astype(F32)).astype(BF)
    slot = lax.broadcasted_iota(jnp.int32, (tokens, capacity), 1).astype(F32)
    source = lax.broadcasted_iota(jnp.int32, (128, capacity), 0)
    total = None
    for place in range(2 * len(steps)):
        expert = (chip ^ steps[place // 2]) * 2 + (core ^ (place % 2))
        pick = jnp.where(source == expert, 1.0, 0.0).astype(BF)
        taken = dot(slot_of, pick) == slot
        spread = [jnp.where(taken, dot(scales, pick), 0.0).astype(BF) for scales in (high, low)]
        if place < len(pieces):
            for part in spread:
                term = dot(part, pieces[place][...])
                total = term if total is None else total + term
        else:
            column = (place - len(pieces)) * capacity
            high_ref[:, column : column + capacity] = spread[0]
            low_ref[:, column : column + capacity] = spread[1]
    sum_ref[...] = total


def combine(routes, weights, steps, late, pieces):
    tokens, columns = routes.shape[0], pieces[0].shape[1]
    capacity = pieces[0].shape[0]
    return pl.pallas_call(
        functools.partial(combine_kernel, steps, late),
        out_shape=[
            jax.ShapeDtypeStruct((tokens, columns), F32),
            jax.ShapeDtypeStruct((tokens, 2 * late * capacity), BF),
            jax.ShapeDtypeStruct((tokens, 2 * late * capacity), BF),
        ],
        in_specs=whole_specs(2 + len(pieces)),
        out_specs=whole_specs(3),
        compiler_params=kernel_params(8),
        cost_estimate=pl.CostEstimate(
            flops=4 * len(pieces) * tokens * capacity * columns,
            bytes_accessed=2 * MIB,
            transcendentals=0,
        ),
        name="combine",
    )(routes.T, weights.T, *pieces)


def finish_kernel(sum_ref, high_ref, low_ref, *refs):
    pieces, out_ref = refs[:-1], refs[-1]
    total = sum_ref[...]
    for place, ref in enumerate(pieces):
        rows = ref.shape[0]
        for scales in (high_ref, low_ref):
            total = total + dot(scales[:, place * rows : (place + 1) * rows], ref[...])
    out_ref[...] = total.astype(BF)


def finish(total, high, low, pieces):
    return pl.pallas_call(
        finish_kernel,
        out_shape=jax.ShapeDtypeStruct(total.shape, BF),
        in_specs=whole_specs(3 + len(pieces)),
        out_specs=pl.BlockSpec(memory_space=pltpu.VMEM),
        compiler_params=kernel_params(8),
        cost_estimate=pl.CostEstimate(flops=16 * MIB, bytes_accessed=MIB, transcendentals=0),
        name="finish",
    )(total, high, low, *pieces)


def attention_kernel(q_ref, k_ref, v_ref, rim_ref, sink_ref, freq_ref, out_ref, k_all, v_all):
    rows, columns = q_ref.shape
    heads = columns // HD
    group = lax.axis_index("tp") * heads // (HEADS // KV)
    half = HD // 2
    lanes = k_ref.shape[1]
    packed = freq_ref.shape[1] // half
    lines = (WINDOW + rows) // packed
    row = lax.broadcasted_iota(jnp.int32, (lines, packed * half), 0)
    part = lax.broadcasted_iota(jnp.int32, (lines, packed * half), 1) // half
    position = lax.axis_index("ep") * rows - WINDOW + part * lines + row
    angles = position.astype(F32) * freq_ref[...]
    tables = []
    for table in (jnp.cos(angles), jnp.sin(angles)):
        tables.append(jnp.concatenate([table[:, i * half : (i + 1) * half] for i in range(packed)], 0))

    def rotated(value, start, count):
        size = value.shape[1]
        row = lax.broadcasted_iota(jnp.int32, (size, size), 0)
        column = lax.broadcasted_iota(jnp.int32, (size, size), 1)
        upper = lax.rem(column, HD) >= half
        swap = jnp.where(upper & (row == column - half), 1.0, 0.0)
        swap = jnp.where(jnp.logical_not(upper) & (row == column + half), -1.0, swap)
        cosine, sine = [table[start : start + count, :] for table in tables]
        copies = size // half
        cosine, sine = jnp.concatenate([cosine] * copies, 1), jnp.concatenate([sine] * copies, 1)
        return value.astype(F32) * cosine + dot(value, swap.astype(BF)) * sine

    def grouped(value):
        picked = value[:, :HD]
        for index in range(1, KV):
            picked = jnp.where(group == index, value[:, index * HD : (index + 1) * HD], picked)
        return picked

    k_all[:WINDOW, :] = grouped(rotated(rim_ref[:, :lanes], 0, WINDOW)).astype(BF)
    k_all[WINDOW:, :] = grouped(rotated(k_ref[...], WINDOW, rows)).astype(BF)
    v_all[:WINDOW, :] = grouped(rim_ref[:, lanes:].astype(F32)).astype(BF)
    v_all[WINDOW:, :] = grouped(v_ref[...].astype(F32)).astype(BF)
    query = (rotated(q_ref[...], WINDOW, rows).astype(BF).astype(F32) * HD**-0.5).astype(BF)
    stacked = heads * WINDOW
    line = lax.broadcasted_iota(jnp.int32, (stacked, 2 * WINDOW), 0)
    key_at = lax.broadcasted_iota(jnp.int32, (stacked, 2 * WINDOW), 1)
    distance = lax.rem(line, WINDOW) + WINDOW - key_at
    near = (distance >= 0) & (distance < WINDOW)
    inside = near & ((key_at >= WINDOW) | (lax.axis_index("ep") > 0))
    head_of = lax.broadcasted_iota(jnp.int32, (stacked, 1), 0) // WINDOW
    sink = jnp.full((stacked, 1), sink_ref[0], F32)
    for head in range(1, heads):
        sink = jnp.where(head_of == head, sink_ref[head], sink)
    for block in range(rows // WINDOW):
        start = block * WINDOW
        band = pl.ds(start, 2 * WINDOW)
        lines = [query[start : start + WINDOW, h * HD : (h + 1) * HD] for h in range(heads)]
        scores = lax.dot_general(
            jnp.concatenate(lines, 0), k_all[band, :], (((1,), (1,)), ((), ())), preferred_element_type=F32
        )
        scores = jnp.where(near if block else inside, scores, mask_value)
        top = jnp.maximum(jnp.max(scores, axis=1, keepdims=True), sink)
        spread = jnp.exp(scores - top)
        total = jnp.sum(spread, axis=1, keepdims=True) + jnp.exp(sink - top)
        mix = dot((spread * (1.0 / total)).astype(BF), v_all[band, :])
        mixes = [mix[h * WINDOW : (h + 1) * WINDOW, :] for h in range(heads)]
        out_ref[start : start + WINDOW, :] = jnp.concatenate(mixes, 1).astype(BF)


def attention(queries, keys, values, rim, sink_logits):
    rows, columns = queries.shape
    half = HD // 2
    packed = 128 // half
    inv_freq = 10000.0 ** (-np.arange(half, dtype=np.float64) * (2.0 / HD))
    inv_freq = np.tile(inv_freq.astype(np.float32)[None, :], (1, packed))
    return pl.pallas_call(
        attention_kernel,
        out_shape=jax.ShapeDtypeStruct((rows, columns), BF),
        in_specs=whole_specs(4) + [pl.BlockSpec(memory_space=pltpu.SMEM)] + whole_specs(1),
        out_specs=pl.BlockSpec(memory_space=pltpu.VMEM),
        scratch_shapes=[pltpu.VMEM((WINDOW + rows, HD), BF)] * 2,
        compiler_params=kernel_params(12),
        cost_estimate=pl.CostEstimate(
            flops=16 * rows * columns * 2 * WINDOW, bytes_accessed=2 * MIB, transcendentals=0
        ),
        name="attention",
    )(queries, keys, values, rim, sink_logits, jnp.asarray(inv_freq))


def fold_kernel(second_ref, near_ref, out_ref):
    width = out_ref.shape[1]
    out_ref[...] = (second_ref[...].astype(F32) + near_ref[:, width:].astype(F32)).astype(BF)


def fold(second, near):
    return pl.pallas_call(
        fold_kernel,
        out_shape=jax.ShapeDtypeStruct(second.shape, BF),
        in_specs=whole_specs(2),
        out_specs=pl.BlockSpec(memory_space=pltpu.VMEM),
        compiler_params=kernel_params(4),
        cost_estimate=pl.CostEstimate(flops=MIB, bytes_accessed=MIB, transcendentals=0),
        name="fold",
    )(second, near)


def local_planes(
    queries,
    keys,
    values,
    sink_logits,
    out_weight,
    expert_input,
    norm_gain,
    routes,
    route_weights,
    gate_weight,
    up_weight,
    down_weight,
):
    n_ep, n_tp = lax.axis_size("ep"), lax.axis_size("tp")
    chips = n_ep // 2
    token_rows, features = expert_input.shape
    capacity = 2 * routes.shape[1] * token_rows // n_ep
    width = features // n_tp

    def in_plane(value, order):
        pairs = []
        for device in range(n_ep):
            step = 1 + (device + order) % 2
            pairs += [(device * n_tp + i, device * n_tp + (i ^ step)) for i in range(n_tp)]
        return lax.ppermute(value, ("ep", "tp"), pairs)

    def along(value, mask):
        return lax.ppermute(value, "ep", [(i, i ^ mask) for i in range(n_ep)])

    def gathered(value):
        near = in_plane(value, 0)
        return value, near, in_plane(value, 1), in_plane(near, 1)

    def scattered(mine, second, far):
        near = in_plane(far, 0)
        summed = fold(second, near)
        last = in_plane(summed, 1)
        return settle(mine, near, last)

    weights = (gate_weight, up_weight, down_weight)
    steps = tuple(range(chips - 1, 0, -1))
    sent = dispatch(expert_input, norm_gain, routes, queries, keys, values, capacity, chips, width)
    sent, (mine, other, rim), local = sent[:-6], sent[-6:-3], sent[-3:]
    rim = passed_along(rim, "ep", 1)
    own = [mine, along(other, 1)]
    arrived = {}
    for step in steps:
        pair = [along(sent[2 * (chips - 1 - step) + i], 2 * step) for i in range(2)]
        arrived[step] = [pair[0], along(pair[1], 1)]
    head_mix = attention(*local, rim, sink_logits)
    parts = gathered(head_mix)
    attn_out = project(parts, out_weight)
    outcome = experts(own, weights, width, 4, fetch=True)
    weights, outcome = outcome[:3], outcome[3:]
    same, cross = scattered(*outcome)
    pieces = {0: [same, along(cross, 1)]}
    for step in steps:
        rows = arrived[step]
        if step > NEAR:
            rows = join(*rows)
            rows = gathered(rows)
        outcome = experts(rows, weights, width, 4)
        same, cross = scattered(*outcome)
        cross = along(cross, 1)
        pieces[step] = [along(same, 2 * step), along(cross, 2 * step)]
    turns = steps + (0,)
    early = [piece for step in turns[:-LATE] for piece in pieces[step]]
    tail = [piece for step in turns[-LATE:] for piece in pieces[step]]
    so_far = combine(routes, route_weights, turns, LATE, early)
    expert_out = finish(*so_far, tail)
    return (attn_out, expert_out)


def local_of(mesh):
    chips = mesh.shape["ep"] // 2
    paired = mesh.shape["ep"] == 2 * chips and chips & (chips - 1) == 0
    return local_planes if mesh.shape["tp"] == 4 and paired else local_general


def solution(mesh):
    return jax.shard_map(
        local_of(mesh),
        mesh=mesh,
        in_specs=(
            P("ep", "tp"),
            P("ep", None),
            P("ep", None),
            P("tp"),
            P(None, "tp"),
            P("ep", None),
            P(),
            P("ep", None),
            P("ep", None),
            P("ep", None, "tp"),
            P("ep", None, "tp"),
            P("ep", "tp", None),
        ),
        out_specs=(P("ep", "tp"), P("ep", "tp")),
        check_vma=False,
    )
```

```python
import functools

import jax
import jax.numpy as jnp
import numpy as np
from jax import lax
from jax.experimental import pallas as pl
from jax.experimental.pallas import tpu as pltpu
from jax.sharding import PartitionSpec as P


HEADS = 16
KV = 2
HD = 64
WINDOW = 128


rms_eps = 1e-06
mask_value = -1e30


def passed_along(value, axis, steps):
    count = lax.axis_size(axis)
    first, last = (max(0, -steps), min(count, count - steps))
    return lax.ppermute(value, axis, [(source, source + steps) for source in range(first, last)])


def rotate_heads(values_in, positions):
    half_dim = values_in.shape[-1] // 2
    inv_freq = 10000.0 ** (-jnp.arange(half_dim, dtype=jnp.float32) * (2.0 / values_in.shape[-1]))
    angles = positions[:, None] * inv_freq[None, :]
    cosine_table = jnp.cos(angles)[:, None, :]
    sine_table = jnp.sin(angles)[:, None, :]
    first_half = values_in[..., :half_dim]
    second_half = values_in[..., half_dim:]
    return jnp.concatenate(
        [
            first_half * cosine_table - second_half * sine_table,
            second_half * cosine_table + first_half * sine_table,
        ],
        axis=-1,
    )


def local_general(
    queries,
    keys,
    values,
    sink_logits,
    out_weight,
    expert_input,
    norm_gain,
    routes,
    route_weights,
    gate_weight,
    up_weight,
    down_weight,
):
    seq_rows = queries.shape[0]
    heads_here = queries.shape[1] // HD
    group_size = HEADS // KV
    kv_here = max(1, heads_here // group_size)
    heads_per_kv = heads_here // kv_here
    kv_first = lax.axis_index("tp") * heads_here // group_size
    key_local = lax.dynamic_slice_in_dim(keys, kv_first * HD, kv_here * HD, 1)
    value_local = lax.dynamic_slice_in_dim(values, kv_first * HD, kv_here * HD, 1)
    offset = lax.axis_index("ep") * seq_rows
    positions = (offset + jnp.arange(seq_rows, dtype=jnp.int32)).astype(jnp.float32)
    query_rot = rotate_heads(
        queries.astype(jnp.float32).reshape(seq_rows, heads_here, HD), positions
    ).astype(jnp.bfloat16)
    key_rot = rotate_heads(
        key_local.astype(jnp.float32).reshape(seq_rows, kv_here, HD), positions
    ).astype(jnp.bfloat16)
    value_heads = value_local.reshape(seq_rows, kv_here, HD)
    rim_pair = jnp.concatenate(
        [
            key_rot.reshape(seq_rows, kv_here * HD)[seq_rows - WINDOW :],
            value_local[seq_rows - WINDOW :],
        ],
        axis=1,
    )
    rim_pair = passed_along(rim_pair, "ep", 1)
    rim_key = rim_pair[:, : kv_here * HD].reshape(WINDOW, kv_here, HD)
    rim_value = rim_pair[:, kv_here * HD :].reshape(WINDOW, kv_here, HD)
    blocks = seq_rows // WINDOW

    def band_of(rim_part, local_part):
        padded = jnp.concatenate([rim_part, local_part], axis=0)
        earlier = padded[:seq_rows].reshape(blocks, WINDOW, kv_here, HD)
        current = padded[WINDOW:].reshape(blocks, WINDOW, kv_here, HD)
        return jnp.concatenate([earlier, current], axis=1)

    key_band = band_of(rim_key, key_rot)
    value_band = band_of(rim_value, value_heads)
    query_blocks = query_rot.reshape(blocks, WINDOW, kv_here, heads_per_kv, HD)
    scores = jnp.einsum(
        "nqhgd,nkhd->nhgqk", query_blocks, key_band, preferred_element_type=jnp.float32
    ) * HD ** (-0.5)
    block_start = offset + jnp.arange(blocks, dtype=jnp.int32)[:, None, None] * WINDOW
    query_pos = block_start + jnp.arange(WINDOW, dtype=jnp.int32)[None, :, None]
    key_pos = block_start - WINDOW + jnp.arange(2 * WINDOW, dtype=jnp.int32)[None, None, :]
    distance = query_pos - key_pos
    allowed = (distance >= 0) & (distance < WINDOW) & (key_pos >= 0)
    scores = jnp.where(allowed[:, None, None], scores, mask_value)
    sink_row = sink_logits.reshape(1, kv_here, heads_per_kv, 1)
    row_top = jnp.maximum(jnp.max(scores, axis=-1), sink_row)
    exp_scores = jnp.exp(scores - row_top[..., None])
    row_total = jnp.sum(exp_scores, axis=-1) + jnp.exp(sink_row - row_top)
    weights = (exp_scores / row_total[..., None]).astype(jnp.bfloat16)
    head_mix = jnp.einsum(
        "nhgqk,nkhd->nqhgd", weights, value_band, preferred_element_type=jnp.float32
    )
    head_mix = head_mix.astype(jnp.bfloat16).reshape(seq_rows, heads_here * HD)
    attn_out = jnp.dot(
        lax.all_gather(head_mix, "tp", axis=1, tiled=True),
        out_weight,
        preferred_element_type=jnp.float32,
    ).astype(jnp.bfloat16)
    token_rows = expert_input.shape[0]
    top_count = routes.shape[1]
    expert_count = lax.axis_size("ep")
    capacity = 2 * top_count * token_rows // expert_count
    slot_total = expert_count * capacity
    input_wide = expert_input.astype(jnp.float32)
    inv_rms = lax.rsqrt(jnp.mean(input_wide * input_wide, axis=-1, keepdims=True) + rms_eps)
    normed = (input_wide * inv_rms * norm_gain[None, :]).astype(jnp.bfloat16)
    flat_expert = routes.reshape(-1)
    one_hot = (flat_expert[:, None] == jnp.arange(expert_count, dtype=jnp.int32)[None, :]).astype(
        jnp.int32
    )
    route_rank = jnp.sum(jnp.cumsum(one_hot, axis=0) * one_hot, axis=1) - 1
    slot_of_route = flat_expert * capacity + route_rank
    matches = slot_of_route[None, :] == jnp.arange(slot_total, dtype=jnp.int32)[:, None]
    route_token = jnp.arange(token_rows * top_count, dtype=jnp.int32) // top_count
    source_row = jnp.sum(jnp.where(matches, route_token[None, :] + 1, 0), axis=1) - 1
    occupied = source_row >= 0
    gate_local = gate_weight[0]
    up_local = up_weight[0]
    down_local = down_weight[0]
    column_count = normed.shape[1] // lax.axis_size("tp")
    own_columns = lax.dynamic_slice_in_dim(
        normed, lax.axis_index("tp") * column_count, column_count, 1
    )
    slot_rows = jnp.where(
        occupied[:, None],
        jnp.take(own_columns, jnp.maximum(source_row, 0), axis=0),
        jnp.zeros((), jnp.bfloat16),
    )
    outgoing = slot_rows.reshape(expert_count, capacity, column_count)
    arrived = lax.all_to_all(outgoing, "ep", split_axis=0, concat_axis=0, tiled=True)
    leading = arrived.shape[:2]
    portion = lax.all_gather(arrived, "tp", axis=2, tiled=True)
    flat_piece = portion.reshape(-1, portion.shape[2])
    gate_acc = jnp.dot(flat_piece, gate_local, preferred_element_type=jnp.float32)
    up_acc = jnp.dot(flat_piece, up_local, preferred_element_type=jnp.float32)
    hidden = (jax.nn.silu(gate_acc) * up_acc).astype(jnp.bfloat16)
    summed = lax.psum_scatter(
        lax.dot_general(
            down_local, hidden, (((0,), (1,)), ((), ())), preferred_element_type=jnp.float32
        ).astype(jnp.bfloat16),
        "tp",
        scatter_dimension=0,
        tiled=True,
    ).astype(jnp.float32)
    returned = summed.astype(jnp.bfloat16).reshape((summed.shape[0],) + leading)
    results_home = lax.all_to_all(returned, "ep", split_axis=1, concat_axis=1, tiled=True)
    home_flat = results_home.reshape(results_home.shape[0], -1)
    picked = jnp.take(home_flat, slot_of_route, axis=1).astype(jnp.float32)
    weighted = picked * route_weights.reshape(1, -1)
    combined = jnp.sum(weighted.reshape(results_home.shape[0], token_rows, top_count), axis=2)
    expert_out = combined.T.astype(jnp.bfloat16)
    return (attn_out, expert_out)


BF = jnp.bfloat16
F32 = jnp.float32
MIB = 1024 * 1024
LATE = 2
NEAR = 1


def dot(left, right):
    return jnp.dot(left, right, preferred_element_type=F32)


def quarter(index, width):
    return pl.ds(pl.multiple_of(index * width, width), width)


def kernel_params(limit_mib, **extra):
    return pltpu.CompilerParams(vmem_limit_bytes=limit_mib * MIB, **extra)


def in_hbm(*values):
    return [pltpu.with_memory_space_constraint(value, pltpu.HBM) for value in values]


def whole_specs(count):
    return [pl.BlockSpec(memory_space=pltpu.VMEM)] * count


def axes_here():
    first = 1 + lax.rem(lax.axis_index("ep"), 2)
    return first, 3 - first


def naming(routes, lanes):
    choices, tokens = routes.shape
    expert = lax.broadcasted_iota(jnp.int32, (lanes, tokens), 0)
    hit = routes[0:1, :] == expert
    for choice in range(1, choices):
        hit = hit | (routes[choice : choice + 1, :] == expert)
    named = jnp.where(hit, 1.0, 0.0).astype(BF)
    row = lax.broadcasted_iota(jnp.int32, (tokens, tokens), 0)
    column = lax.broadcasted_iota(jnp.int32, (tokens, tokens), 1)
    earlier = jnp.where(row < column, 1.0, 0.0).astype(BF)
    return jnp.where(hit, dot(named, earlier), -1.0)


def dispatch_kernel(capacity, chips, x_hbm, gain_hbm, routes_hbm, queries_hbm, keys_hbm, values_hbm, *refs):
    outs, (x, gain, routes, normed, slot_of, arrival) = refs[:-6], refs[-6:]
    lanes = keys_hbm.shape[1]
    tail = pl.ds(keys_hbm.shape[0] - WINDOW, WINDOW)
    rim, queries, keys, values = outs[-4:]
    moves = (
        (routes_hbm, routes),
        (x_hbm, x),
        (gain_hbm, gain),
        (keys_hbm.at[tail, :], rim.at[:, :lanes]),
        (values_hbm.at[tail, :], rim.at[:, lanes:]),
        (queries_hbm, queries),
        (keys_hbm, keys),
        (values_hbm, values),
    )
    copies = [pltpu.make_async_copy(s, d, arrival.at[i]) for i, (s, d) in enumerate(moves)]
    for copy in copies:
        copy.start()
    me = lax.axis_index("ep")
    chip, core = me // 2, lax.rem(me, 2)
    tokens = x.shape[0]
    copies[0].wait()
    slot_of[...] = naming(routes[...], slot_of.shape[0])
    copies[1].wait()
    copies[2].wait()
    wide = x[...].astype(F32)
    inv_rms = lax.rsqrt(jnp.mean(wide * wide, axis=-1, keepdims=True) + rms_eps)
    normed[...] = (wide * inv_rms * gain[...]).astype(BF)
    slot = lax.broadcasted_iota(jnp.int32, (capacity, tokens), 0).astype(F32)

    def chosen(expert):
        return jnp.where(slot_of[pl.ds(expert, 1), :] == slot, 1.0, 0.0).astype(BF)

    width = outs[0].shape[1]
    share = normed[:, quarter(lax.axis_index("tp"), width)]
    place = 0
    for step in range(chips - 1, -1, -1):
        for other in range(2):
            rows = share if step > NEAR else normed[...]
            expert = (chip ^ step) * 2 + (core ^ other)
            outs[place][...] = dot(chosen(expert), rows).astype(BF)
            place += 1
    for copy in copies[3:]:
        copy.wait()


def dispatch(x, gain, routes, queries, keys, values, capacity, chips, width):
    tokens, features = x.shape
    shapes = [(capacity, width if i < 2 * (chips - 1 - NEAR) else features) for i in range(2 * chips)]
    shapes += [(WINDOW, 2 * keys.shape[1]), queries.shape, keys.shape, values.shape]
    return pl.pallas_call(
        functools.partial(dispatch_kernel, capacity, chips),
        out_shape=[jax.ShapeDtypeStruct(s, BF) for s in shapes],
        in_specs=[pl.BlockSpec(memory_space=pltpu.HBM)] * 6,
        out_specs=whole_specs(len(shapes)),
        scratch_shapes=[
            pltpu.VMEM((tokens, features), BF),
            pltpu.VMEM((1, features), F32),
            pltpu.VMEM(routes.shape[::-1], jnp.int32),
            pltpu.VMEM((tokens, features), BF),
            pltpu.VMEM((8 * -(-2 * chips // 8), tokens), F32),
            pltpu.SemaphoreType.DMA((8,)),
        ],
        compiler_params=kernel_params(24),
        cost_estimate=pl.CostEstimate(
            flops=4 * capacity * tokens * features * 2, bytes_accessed=4 * MIB, transcendentals=0
        ),
        name="dispatch",
    )(*in_hbm(x, gain.reshape(1, -1), routes.T, queries, keys, values))


def experts_kernel(split, fetch, blocks, *refs):
    count = 4 if split else 2
    rows_in = refs[:count]
    x, hidden = refs[-2:]
    if not fetch:
        gate, up, down, *outs = refs[count:-2]
    else:
        gate_hbm, up_hbm, down_hbm, gate, up, down, *outs, arrival = refs[count:-2]
    here = lax.axis_index("tp")
    first, second = axes_here()
    width = outs[0].shape[1]
    block = hidden.shape[1] // blocks
    parts = [pl.ds(step * block, block) for step in range(blocks)]
    quarters = [quarter(index, width) for index in (here ^ 3, here ^ first, here ^ second, here)]
    copies = []
    if fetch:
        for place, part in enumerate(parts):
            for source, target, row in ((gate_hbm, gate, 0), (up_hbm, up, 1)):
                copies.append(
                    pltpu.make_async_copy(
                        source.at[:, :, part], target.at[:, :, part], arrival.at[row, place]
                    )
                )
        for place, part in enumerate(quarters):
            copies.append(
                pltpu.make_async_copy(down_hbm.at[:, :, part], down.at[:, :, part], arrival.at[2, place])
            )
        for copy in copies:
            copy.start()
    if split:
        for ref, index in zip(rows_in, (here, here ^ first, here ^ second, here ^ 3)):
            x[:, quarter(index, width)] = ref[...]
    else:
        half = rows_in[0].shape[0]
        x[:half, :] = rows_in[0][...]
        x[half:, :] = rows_in[1][...]
    for place, part in enumerate(parts):
        for copy in copies[2 * place : 2 * place + 2]:
            copy.wait()
        gated = dot(x[...], gate[0, :, part])
        upped = dot(x[...], up[0, :, part])
        hidden[:, part] = (gated / (1.0 + jnp.exp(-gated)) * upped).astype(BF)
    for place, part in enumerate(quarters):
        for copy in copies[2 * blocks + place : 2 * blocks + place + 1]:
            copy.wait()
        outs[3 - place][...] = dot(hidden[...], down[0, :, part]).astype(BF)


def experts(rows_in, weights, width, blocks, fetch=False):
    split = len(rows_in) == 4
    rows = rows_in[0].shape[0] if split else 2 * rows_in[0].shape[0]
    _, features, hidden = weights[0].shape
    out_shape = [jax.ShapeDtypeStruct((rows, width), BF)] * 4
    scratch = [pltpu.VMEM((rows, features), BF), pltpu.VMEM((rows, hidden), BF)]
    weight_specs = whole_specs(3)
    if fetch:
        weights = in_hbm(*weights)
        out_shape = [jax.ShapeDtypeStruct(w.shape, w.dtype) for w in weights] + out_shape
        weight_specs = [pl.BlockSpec(memory_space=pltpu.HBM)] * 3
        scratch = [pltpu.SemaphoreType.DMA((3, max(4, blocks)))] + scratch
    return pl.pallas_call(
        functools.partial(experts_kernel, split, fetch, blocks),
        out_shape=out_shape,
        in_specs=whole_specs(len(rows_in)) + weight_specs,
        out_specs=whole_specs(len(out_shape)),
        scratch_shapes=scratch,
        compiler_params=kernel_params(24 if fetch else 8),
        cost_estimate=pl.CostEstimate(
            flops=6 * rows * features * hidden,
            bytes_accessed=6 * features * hidden,
            transcendentals=rows * hidden,
        ),
        name="experts",
    )(*rows_in, *weights)


def join_kernel(top_ref, bottom_ref, out_ref):
    rows = top_ref.shape[0]
    out_ref[:rows, :] = top_ref[...]
    out_ref[rows:, :] = bottom_ref[...]


def join(top, bottom):
    rows, columns = top.shape
    return pl.pallas_call(
        join_kernel,
        out_shape=jax.ShapeDtypeStruct((2 * rows, columns), top.dtype),
        in_specs=whole_specs(2),
        out_specs=pl.BlockSpec(memory_space=pltpu.VMEM),
        compiler_params=kernel_params(2),
        cost_estimate=pl.CostEstimate(flops=MIB, bytes_accessed=MIB, transcendentals=0),
        name="join",
    )(top, bottom)


def settle_kernel(mine_ref, near_ref, last_ref, same_ref, cross_ref):
    rows, _ = same_ref.shape
    for out_ref, start in ((same_ref, 0), (cross_ref, rows)):
        part = pl.ds(start, rows)
        total = mine_ref[part, :].astype(F32) + near_ref[part, :].astype(F32)
        out_ref[...] = (total + last_ref[part, :].astype(F32)).astype(BF)


def settle(mine, near, last):
    rows, width = mine.shape
    return pl.pallas_call(
        settle_kernel,
        out_shape=[jax.ShapeDtypeStruct((rows // 2, width), BF)] * 2,
        in_specs=whole_specs(3),
        out_specs=whole_specs(2),
        compiler_params=kernel_params(4),
        cost_estimate=pl.CostEstimate(flops=MIB, bytes_accessed=MIB, transcendentals=0),
        name="settle",
    )(mine, near, last)


def project_kernel(*refs):
    parts, (weight_ref, out_ref) = refs[:4], refs[4:]
    here = lax.axis_index("tp")
    first, second = axes_here()
    depth = parts[0].shape[1]
    total = None
    for ref, index in zip(parts, (here, here ^ first, here ^ second, here ^ 3)):
        term = dot(ref[...], weight_ref[quarter(index, depth), :])
        total = term if total is None else total + term
    out_ref[...] = total.astype(BF)


def project(parts, weight):
    rows, columns = parts[0].shape[0], weight.shape[1]
    return pl.pallas_call(
        project_kernel,
        out_shape=jax.ShapeDtypeStruct((rows, columns), BF),
        in_specs=whole_specs(5),
        out_specs=pl.BlockSpec(memory_space=pltpu.VMEM),
        compiler_params=kernel_params(8),
        cost_estimate=pl.CostEstimate(
            flops=2 * rows * weight.shape[0] * columns, bytes_accessed=3 * MIB, transcendentals=0
        ),
        name="project",
    )(*parts, weight)


def combine_kernel(steps, late, *refs):
    routes_ref, weights_ref = refs[:2]
    pieces, (sum_ref, high_ref, low_ref) = refs[2:-3], refs[-3:]
    me = lax.axis_index("ep")
    chip, core = me // 2, lax.rem(me, 2)
    routes = routes_ref[...]
    choices, tokens = routes.shape
    capacity = high_ref.shape[1] // (2 * late)
    slot_of = naming(routes, 128)
    row = lax.broadcasted_iota(jnp.int32, (128, tokens), 0)
    scale = jnp.zeros((128, tokens), F32)
    for choice in range(choices):
        scale = jnp.where(routes[choice : choice + 1, :] == row, weights_ref[choice : choice + 1, :], scale)
    slot_of = slot_of.T.astype(BF)
    scale = scale.T
    high = scale.astype(BF)
    low = (scale - high.astype(F32)).astype(BF)
    slot = lax.broadcasted_iota(jnp.int32, (tokens, capacity), 1).astype(F32)
    source = lax.broadcasted_iota(jnp.int32, (128, capacity), 0)
    total = None
    for place in range(2 * len(steps)):
        expert = (chip ^ steps[place // 2]) * 2 + (core ^ (place % 2))
        pick = jnp.where(source == expert, 1.0, 0.0).astype(BF)
        taken = dot(slot_of, pick) == slot
        spread = [jnp.where(taken, dot(scales, pick), 0.0).astype(BF) for scales in (high, low)]
        if place < len(pieces):
            for part in spread:
                term = dot(part, pieces[place][...])
                total = term if total is None else total + term
        else:
            column = (place - len(pieces)) * capacity
            high_ref[:, column : column + capacity] = spread[0]
            low_ref[:, column : column + capacity] = spread[1]
    sum_ref[...] = total


def combine(routes, weights, steps, late, pieces):
    tokens, columns = routes.shape[0], pieces[0].shape[1]
    capacity = pieces[0].shape[0]
    return pl.pallas_call(
        functools.partial(combine_kernel, steps, late),
        out_shape=[
            jax.ShapeDtypeStruct((tokens, columns), F32),
            jax.ShapeDtypeStruct((tokens, 2 * late * capacity), BF),
            jax.ShapeDtypeStruct((tokens, 2 * late * capacity), BF),
        ],
        in_specs=whole_specs(2 + len(pieces)),
        out_specs=whole_specs(3),
        compiler_params=kernel_params(8),
        cost_estimate=pl.CostEstimate(
            flops=4 * len(pieces) * tokens * capacity * columns,
            bytes_accessed=2 * MIB,
            transcendentals=0,
        ),
        name="combine",
    )(routes.T, weights.T, *pieces)


def finish_kernel(sum_ref, high_ref, low_ref, *refs):
    pieces, out_ref = refs[:-1], refs[-1]
    total = sum_ref[...]
    for place, ref in enumerate(pieces):
        rows = ref.shape[0]
        for scales in (high_ref, low_ref):
            total = total + dot(scales[:, place * rows : (place + 1) * rows], ref[...])
    out_ref[...] = total.astype(BF)


def finish(total, high, low, pieces):
    return pl.pallas_call(
        finish_kernel,
        out_shape=jax.ShapeDtypeStruct(total.shape, BF),
        in_specs=whole_specs(3 + len(pieces)),
        out_specs=pl.BlockSpec(memory_space=pltpu.VMEM),
        compiler_params=kernel_params(8),
        cost_estimate=pl.CostEstimate(flops=16 * MIB, bytes_accessed=MIB, transcendentals=0),
        name="finish",
    )(total, high, low, *pieces)


def attention_kernel(q_ref, k_ref, v_ref, rim_ref, sink_ref, freq_ref, out_ref, k_all, v_all):
    rows, columns = q_ref.shape
    heads = columns // HD
    group = lax.axis_index("tp") * heads // (HEADS // KV)
    half = HD // 2
    lanes = k_ref.shape[1]
    packed = freq_ref.shape[1] // half
    lines = (WINDOW + rows) // packed
    row = lax.broadcasted_iota(jnp.int32, (lines, packed * half), 0)
    part = lax.broadcasted_iota(jnp.int32, (lines, packed * half), 1) // half
    position = lax.axis_index("ep") * rows - WINDOW + part * lines + row
    angles = position.astype(F32) * freq_ref[...]
    tables = []
    for table in (jnp.cos(angles), jnp.sin(angles)):
        tables.append(jnp.concatenate([table[:, i * half : (i + 1) * half] for i in range(packed)], 0))

    def rotated(value, start, count):
        size = value.shape[1]
        row = lax.broadcasted_iota(jnp.int32, (size, size), 0)
        column = lax.broadcasted_iota(jnp.int32, (size, size), 1)
        upper = lax.rem(column, HD) >= half
        swap = jnp.where(upper & (row == column - half), 1.0, 0.0)
        swap = jnp.where(jnp.logical_not(upper) & (row == column + half), -1.0, swap)
        cosine, sine = [table[start : start + count, :] for table in tables]
        copies = size // half
        cosine, sine = jnp.concatenate([cosine] * copies, 1), jnp.concatenate([sine] * copies, 1)
        return value.astype(F32) * cosine + dot(value, swap.astype(BF)) * sine

    def grouped(value):
        picked = value[:, :HD]
        for index in range(1, KV):
            picked = jnp.where(group == index, value[:, index * HD : (index + 1) * HD], picked)
        return picked

    k_all[:WINDOW, :] = grouped(rotated(rim_ref[:, :lanes], 0, WINDOW)).astype(BF)
    k_all[WINDOW:, :] = grouped(rotated(k_ref[...], WINDOW, rows)).astype(BF)
    v_all[:WINDOW, :] = grouped(rim_ref[:, lanes:].astype(F32)).astype(BF)
    v_all[WINDOW:, :] = grouped(v_ref[...].astype(F32)).astype(BF)
    query = (rotated(q_ref[...], WINDOW, rows).astype(BF).astype(F32) * HD**-0.5).astype(BF)
    stacked = heads * WINDOW
    line = lax.broadcasted_iota(jnp.int32, (stacked, 2 * WINDOW), 0)
    key_at = lax.broadcasted_iota(jnp.int32, (stacked, 2 * WINDOW), 1)
    distance = lax.rem(line, WINDOW) + WINDOW - key_at
    near = (distance >= 0) & (distance < WINDOW)
    inside = near & ((key_at >= WINDOW) | (lax.axis_index("ep") > 0))
    head_of = lax.broadcasted_iota(jnp.int32, (stacked, 1), 0) // WINDOW
    sink = jnp.full((stacked, 1), sink_ref[0], F32)
    for head in range(1, heads):
        sink = jnp.where(head_of == head, sink_ref[head], sink)
    for block in range(rows // WINDOW):
        start = block * WINDOW
        band = pl.ds(start, 2 * WINDOW)
        lines = [query[start : start + WINDOW, h * HD : (h + 1) * HD] for h in range(heads)]
        scores = lax.dot_general(
            jnp.concatenate(lines, 0), k_all[band, :], (((1,), (1,)), ((), ())), preferred_element_type=F32
        )
        scores = jnp.where(near if block else inside, scores, mask_value)
        top = jnp.maximum(jnp.max(scores, axis=1, keepdims=True), sink)
        spread = jnp.exp(scores - top)
        total = jnp.sum(spread, axis=1, keepdims=True) + jnp.exp(sink - top)
        mix = dot((spread * (1.0 / total)).astype(BF), v_all[band, :])
        mixes = [mix[h * WINDOW : (h + 1) * WINDOW, :] for h in range(heads)]
        out_ref[start : start + WINDOW, :] = jnp.concatenate(mixes, 1).astype(BF)


def attention(queries, keys, values, rim, sink_logits):
    rows, columns = queries.shape
    half = HD // 2
    packed = 128 // half
    inv_freq = 10000.0 ** (-np.arange(half, dtype=np.float64) * (2.0 / HD))
    inv_freq = np.tile(inv_freq.astype(np.float32)[None, :], (1, packed))
    return pl.pallas_call(
        attention_kernel,
        out_shape=jax.ShapeDtypeStruct((rows, columns), BF),
        in_specs=whole_specs(4) + [pl.BlockSpec(memory_space=pltpu.SMEM)] + whole_specs(1),
        out_specs=pl.BlockSpec(memory_space=pltpu.VMEM),
        scratch_shapes=[pltpu.VMEM((WINDOW + rows, HD), BF)] * 2,
        compiler_params=kernel_params(12),
        cost_estimate=pl.CostEstimate(
            flops=16 * rows * columns * 2 * WINDOW, bytes_accessed=2 * MIB, transcendentals=0
        ),
        name="attention",
    )(queries, keys, values, rim, sink_logits, jnp.asarray(inv_freq))


def fold_kernel(second_ref, near_ref, out_ref):
    out_ref[...] = (second_ref[...].astype(F32) + near_ref[...].astype(F32)).astype(BF)


def fold(second, near):
    return pl.pallas_call(
        fold_kernel,
        out_shape=jax.ShapeDtypeStruct(second.shape, BF),
        in_specs=whole_specs(2),
        out_specs=pl.BlockSpec(memory_space=pltpu.VMEM),
        compiler_params=kernel_params(4),
        cost_estimate=pl.CostEstimate(flops=MIB, bytes_accessed=MIB, transcendentals=0),
        name="fold",
    )(second, near)


def local_planes(
    queries,
    keys,
    values,
    sink_logits,
    out_weight,
    expert_input,
    norm_gain,
    routes,
    route_weights,
    gate_weight,
    up_weight,
    down_weight,
):
    n_ep, n_tp = lax.axis_size("ep"), lax.axis_size("tp")
    chips = n_ep // 2
    token_rows, features = expert_input.shape
    capacity = 2 * routes.shape[1] * token_rows // n_ep
    width = features // n_tp

    def in_plane(value, order):
        pairs = []
        for device in range(n_ep):
            step = 1 + (device + order) % 2
            pairs += [(device * n_tp + i, device * n_tp + (i ^ step)) for i in range(n_tp)]
        return lax.ppermute(value, ("ep", "tp"), pairs)

    def along(value, mask):
        return lax.ppermute(value, "ep", [(i, i ^ mask) for i in range(n_ep)])

    def gathered(value):
        near = in_plane(value, 0)
        return value, near, in_plane(value, 1), in_plane(near, 1)

    def scattered(mine, second, first, both):
        near = in_plane(both, 0)
        last = in_plane(fold(second, near), 1)
        near = in_plane(first, 0)
        return settle(mine, near, last)

    weights = (gate_weight, up_weight, down_weight)
    steps = tuple(range(chips - 1, 0, -1))
    sent = dispatch(expert_input, norm_gain, routes, queries, keys, values, capacity, chips, width)
    sent, (mine, other, rim), local = sent[:-6], sent[-6:-3], sent[-3:]
    rim = passed_along(rim, "ep", 1)
    own = [mine, along(other, 1)]
    arrived = {}
    for step in steps:
        rows = sent[2 * (chips - 1 - step) :]
        arrived[step] = [along(rows[i], 2 * step + i) for i in range(2)]
    head_mix = attention(*local, rim, sink_logits)
    parts = gathered(head_mix)
    attn_out = project(parts, out_weight)
    outcome = experts(own, weights, width, 4, fetch=True)
    weights, outcome = outcome[:3], outcome[3:]
    same, cross = scattered(*outcome)
    pieces = {0: [same, along(cross, 1)]}
    for step in steps:
        rows = arrived[step]
        if step > NEAR:
            rows = join(*rows)
            rows = gathered(rows)
        outcome = experts(rows, weights, width, 4)
        same, cross = scattered(*outcome)
        pieces[step] = [along(same, 2 * step), along(cross, 2 * step + 1)]
    turns = steps + (0,)
    early = [piece for step in turns[:-LATE] for piece in pieces[step]]
    tail = [piece for step in turns[-LATE:] for piece in pieces[step]]
    so_far = combine(routes, route_weights, turns, LATE, early)
    expert_out = finish(*so_far, tail)
    return (attn_out, expert_out)


def local_of(mesh):
    chips = mesh.shape["ep"] // 2
    paired = mesh.shape["ep"] == 2 * chips and chips & (chips - 1) == 0
    return local_planes if mesh.shape["tp"] == 4 and paired else local_general


def solution(mesh):
    return jax.shard_map(
        local_of(mesh),
        mesh=mesh,
        in_specs=(
            P("ep", "tp"),
            P("ep", None),
            P("ep", None),
            P("tp"),
            P(None, "tp"),
            P("ep", None),
            P(),
            P("ep", None),
            P("ep", None),
            P("ep", None, "tp"),
            P("ep", None, "tp"),
            P("ep", "tp", None),
        ),
        out_specs=(P("ep", "tp"), P("ep", "tp")),
        check_vma=False,
    )
```
